512 devices in a mesh: sp: 64 (over z, y), tp: 8 (over x, core).
Axes of the slice: x: 4, y: 8, z: 8, core: 2. Of those that a mesh axis runs over, the one named last changes fastest.
Arguments:
- latent: bfloat16 [16384, 2048], P('sp'), may hold values from -6 to 6
- context: bfloat16 [512, 2048], P('sp'), may hold values from -6 to 6
- cond: bfloat16 [2048], P('sp'), may hold values from -6 to 6
- cond_ctx: bfloat16 [2048], P('sp'), may hold values from -6 to 6
- shift_weight: bfloat16 [2048, 2048], P('sp', 'tp'), may hold values from -0.125 to 0.125
- scale_weight: bfloat16 [2048, 2048], P('sp', 'tp'), may hold values from -0.125 to 0.125
- gate_weight: bfloat16 [2048, 2048], P('sp', 'tp'), may hold values from -0.25 to 0.25
- norm_gain: bfloat16 [2048], replicated, may hold values from 0.099609375 to 1.8984375
- query_weight: bfloat16 [2048, 1024], P(None, 'tp'), may hold values from -0.125 to 0.125
- key_weight: bfloat16 [2048, 1024], P(None, 'tp'), may hold values from -0.125 to 0.125
- value_weight: bfloat16 [2048, 1024], P(None, 'tp'), may hold values from -0.125 to 0.125
- query_gain: bfloat16 [64], replicated, may hold values from 0.099609375 to 1.8984375
- key_gain: bfloat16 [64], replicated, may hold values from 0.099609375 to 1.8984375
- offset_bias: float32 [16, 15, 31], P('tp'), may hold values from -0.5 to 251
- out_weight: bfloat16 [1024, 2048], P(None, 'tp'), may hold values from -1.5 to 1.5
Outputs:
- updated: bfloat16 [16384, 2048], P('sp', 'tp')
The draws below stay inside these ranges and needn't reach their ends.
All inputs are finite; a program needn't handle non-finite values.
Results may differ from the reference program's by a relative error of at most 0.0077.
Values may be sent and summed in bfloat16 or wider, within the bound.
A program may use at most 64 MiB of HBM per device.

```python
import jax
import jax.numpy as jnp
from jax import lax

D = 2048
HEADS = 16
HEAD_DIM = 64
WIN_ROWS = 8
WIN_COLS = 16
GRID_W = 64
CTX = 512
TOKENS = 16384
HD = 1024


def draw_offset_bias(key, part):
    shape = (HEADS, 2 * WIN_ROWS - 1, 2 * WIN_COLS - 1)
    table = jax.random.uniform(jax.random.fold_in(key, 11), shape, jnp.float32, -0.5, 1.0)
    return table


def block_levels(rng, extent, cuts, low, largest):
    def one(position, shards_of):
        heights = jax.random.uniform(jax.random.fold_in(jax.random.fold_in(rng, 6), position), (shards_of,), jnp.float32, low / len(cuts), largest / len(cuts))
        return jnp.repeat(jnp.exp(heights), extent[position] // shards_of).reshape((-1,) + (1,) * (len(extent) - position - 1))

    factor_of = one(*cuts[0])
    for cut in cuts[1:]:
        factor_of = factor_of * one(*cut)
    return factor_of


def gaussian(key, dims, width, limit, shards=(), kind=jnp.bfloat16):
    level = block_levels(key, dims, shards, -0.22, 0.18) if shards else 1.0
    entries = jax.random.normal(key, dims, jnp.float32) * width * level
    return jnp.minimum(jnp.maximum(entries, -limit), limit).astype(kind)


def setup_inputs(seed: int = 0) -> dict:
    splits = jax.random.split(jax.random.key(seed), 16)
    latent = gaussian(splits[0], (TOKENS, D), 1.0, 6.0, ((0, 64),))
    context = gaussian(splits[1], (CTX, D), 1.0, 6.0, ((0, 64),))
    cond = gaussian(splits[2], (D,), 1.0, 6.0, ((0, 64),))
    cond_ctx = gaussian(splits[3], (D,), 1.0, 6.0, ((0, 64),))
    shift_weight = gaussian(splits[4], (D, D), D ** -0.5, 0.125, ((0, 64), (1, 8)))
    scale_weight = gaussian(splits[5], (D, D), D ** -0.5, 0.125, ((0, 64), (1, 8)))
    gate_weight = gaussian(splits[6], (D, D), (D // 4) ** -0.5, 0.25, ((0, 64), (1, 8)))
    norm_gain = jnp.clip(1.0 + 0.18 * jax.random.normal(splits[7], (D,), jnp.float32), 0.099609375, 1.8984375).astype(jnp.bfloat16)
    query_weight = gaussian(splits[8], (D, HD), D ** -0.5, 0.125, ((1, 8),))
    key_weight = gaussian(splits[9], (D, HD), D ** -0.5, 0.125, ((1, 8),))
    value_weight = gaussian(splits[10], (D, HD), D ** -0.5, 0.125, ((1, 8),))
    query_gain = jnp.clip(1.0 + 0.18 * jax.random.normal(splits[11], (HEAD_DIM,), jnp.float32), 0.099609375, 1.8984375).astype(jnp.bfloat16)
    key_gain = jnp.clip(1.0 + 0.18 * jax.random.normal(splits[12], (HEAD_DIM,), jnp.float32), 0.099609375, 1.8984375).astype(jnp.bfloat16)
    offset_bias = draw_offset_bias(jax.random.fold_in(splits[15], 71), 0)
    out_weight = gaussian(splits[14], (HD, D), (max(HD // 64, 1)) ** -0.5, 1.5, ((1, 8),))
    return {"latent": latent, "context": context, "cond": cond, "cond_ctx": cond_ctx, "shift_weight": shift_weight, "scale_weight": scale_weight, "gate_weight": gate_weight, "norm_gain": norm_gain, "query_weight": query_weight, "key_weight": key_weight, "value_weight": value_weight, "query_gain": query_gain, "key_gain": key_gain, "offset_bias": offset_bias, "out_weight": out_weight}


EPS = 1e-06

def modulate(rows, norm_gain, scale, shift):
    values = rows.astype(jnp.float32)
    normed = values * lax.rsqrt(lax.optimization_barrier(jnp.mean(values * values, axis=-1, keepdims=True)) + EPS)
    return (normed * norm_gain.astype(jnp.float32) * (1.0 + scale) + shift).astype(jnp.bfloat16)

def project_heads(hidden, weight, gain):
    raw = jnp.dot(hidden, weight, preferred_element_type=jnp.float32)
    split = raw.reshape(hidden.shape[0], -1, HEAD_DIM)
    if gain is None:
        return split.astype(jnp.bfloat16)
    normed = split * lax.rsqrt(lax.optimization_barrier(jnp.mean(split * split, axis=-1, keepdims=True)) + EPS)
    return (normed * gain.astype(jnp.float32)).astype(jnp.bfloat16)

def reference(latent, context, cond, cond_ctx, shift_weight, scale_weight, gate_weight, norm_gain, query_weight, key_weight, value_weight, query_gain, key_gain, offset_bias, out_weight):
    act = jax.nn.silu(cond.astype(jnp.float32)).astype(jnp.bfloat16)[None, :]
    act_ctx = jax.nn.silu(cond_ctx.astype(jnp.float32)).astype(jnp.bfloat16)[None, :]
    shift = jnp.dot(act, shift_weight, preferred_element_type=jnp.float32)[0]
    scale = jnp.dot(act, scale_weight, preferred_element_type=jnp.float32)[0]
    gate = jnp.dot(act, gate_weight, preferred_element_type=jnp.float32)[0]
    shift_ctx = jnp.dot(act_ctx, shift_weight, preferred_element_type=jnp.float32)[0]
    scale_ctx = jnp.dot(act_ctx, scale_weight, preferred_element_type=jnp.float32)[0]
    hidden = modulate(latent, norm_gain, scale, shift)
    queries = project_heads(hidden, query_weight, query_gain)
    keys = project_heads(hidden, key_weight, key_gain)
    values = project_heads(hidden, value_weight, None)
    hidden_ctx = modulate(context, norm_gain, scale_ctx, shift_ctx)
    ctx_keys = project_heads(hidden_ctx, key_weight, key_gain).astype(jnp.float32)
    ctx_values = project_heads(hidden_ctx, value_weight, None).astype(jnp.float32)
    total_rows = latent.shape[0] // GRID_W
    grid_q = queries.reshape(total_rows, GRID_W, HEADS, HEAD_DIM)
    grid_k = keys.reshape(total_rows, GRID_W, HEADS, HEAD_DIM)
    grid_v = values.reshape(total_rows, GRID_W, HEADS, HEAD_DIM)
    column = jnp.arange(GRID_W, dtype=jnp.int32)
    window_first = jnp.clip(column - WIN_COLS // 2, 0, GRID_W - WIN_COLS)
    inside = (column[None, :] >= window_first[:, None]) & (column[None, :] < window_first[:, None] + WIN_COLS)
    col_offset = jnp.clip(column[None, :] - column[:, None] + WIN_COLS - 1, 0, 2 * WIN_COLS - 2)
    by_col = offset_bias.astype(jnp.float32)[:, :, col_offset]
    factor = HEAD_DIM ** (-0.5)
    band_len = WIN_ROWS * GRID_W

    def one_row(row):
        first = jnp.clip(row - WIN_ROWS // 2, 0, total_rows - WIN_ROWS).astype(jnp.int32)
        band_k = lax.dynamic_slice_in_dim(grid_k, first, WIN_ROWS, 0).astype(jnp.float32)
        band_v = lax.dynamic_slice_in_dim(grid_v, first, WIN_ROWS, 0).astype(jnp.float32)
        query = lax.dynamic_index_in_dim(grid_q, row, 0, keepdims=False).astype(jnp.float32)
        row_offset = (first + jnp.arange(WIN_ROWS, dtype=jnp.int32) - row + WIN_ROWS - 1).astype(jnp.int32)
        bias = jnp.take(by_col, row_offset, axis=1)
        scores = jnp.einsum('qhd,jkhd->hqjk', query, band_k) * factor + jnp.transpose(bias, (0, 2, 1, 3))
        scores = jnp.where(inside[None, :, None, :], scores, -jnp.inf).reshape(HEADS, GRID_W, band_len)
        ctx_scores = jnp.einsum('qhd,chd->hqc', query, ctx_keys) * factor
        weights = jax.nn.softmax(jnp.concatenate([scores, ctx_scores], axis=-1), axis=-1).astype(jnp.bfloat16)
        weights = lax.optimization_barrier(weights).astype(jnp.float32)
        local_w = weights[..., :band_len].reshape(HEADS, GRID_W, WIN_ROWS, GRID_W)
        mixed = jnp.einsum('hqjk,jkhd->qhd', local_w, band_v) + jnp.einsum('hqc,chd->qhd', weights[..., band_len:], ctx_values)
        return mixed.astype(jnp.bfloat16).reshape(GRID_W, HEADS * HEAD_DIM)
    mixed = lax.map(one_row, jnp.arange(total_rows, dtype=jnp.int32)).reshape(latent.shape[0], HEADS * HEAD_DIM)
    projected = jnp.dot(mixed, out_weight, preferred_element_type=jnp.float32)
    return (latent.astype(jnp.float32) + gate[None, :] * projected).astype(jnp.bfloat16)
```

```python
import functools
import math

import jax
import jax.numpy as jnp
from jax import lax
from jax.experimental import pallas as pl
from jax.experimental.pallas import tpu as pltpu
from jax.sharding import Mesh
from jax.sharding import PartitionSpec as P

HEAD_DIM = 64
WIN_ROWS = 8
WIN_COLS = 16
GRID_W = 64
ROWS = 4
TOK = ROWS * GRID_W
LANE = 2 * HEAD_DIM
BLOCK = 256
CTX_DEV = 8
EPS = 1e-06
LOG2E = math.log2(math.e)
NEG = -1e30
SMALL = (2, 3, 7, 11, 12, 13)
AXES = ("z", "y", "x", "c")
MESH = pl.DeviceIdType.MESH
F32 = jnp.float32
BF16 = jnp.bfloat16


def far_first(n):
    return sorted(range(1, n), key=lambda d: -min(d, n - d))


def near_first(n):
    return [0] + sorted(range(1, n), key=lambda d: min(d, n - d))


def dot(a, b):
    return jnp.dot(a, b, preferred_element_type=F32)


def dot_nt(a, b):
    return lax.dot_general(a, b, (((1,), (1,)), ((), ())), preferred_element_type=F32)


def silu(v):
    return v / (1.0 + jnp.exp(-v))


def head_norm(raw, ones_block):
    sq = raw * raw
    hi = sq.astype(BF16)
    lo = (sq - hi.astype(F32)).astype(BF16)
    return raw * lax.rsqrt(dot(hi, ones_block) + dot(lo, ones_block) + EPS)


def kernel(
    sizes,
    latent,
    context,
    cond_hbm,
    cond_ctx_hbm,
    shift_w,
    scale_w,
    gate_w,
    norm_gain_hbm,
    query_w,
    key_w,
    value_w,
    query_gain_hbm,
    key_gain_hbm,
    offset_bias_hbm,
    out_w,
    out,
    lat,
    xn,
    hid,
    w_all,
    wo,
    own,
    craw,
    cxn,
    chid,
    kv,
    kvc,
    qm,
    table,
    top,
    acc,
    bias_rows,
    gains,
    gain_row,
    wmod,
    m1,
    m2,
    g1,
    g2,
    mod,
    mx,
    cond,
    cond_ctx,
    norm_gain,
    query_gain,
    key_gain,
    offset_bias,
    load_sem,
    s1,
    r1,
    s2,
    r2,
    sg1,
    rg1,
    sg2,
    rg2,
    s3,
    r3,
    sc,
    rc,
    sk,
    rk,
    sh,
    rh,
    sm,
    rm,
    sf,
    rf,
):
    nz, ny, nx, nc = sizes
    nsp, ntp = nz * ny, nx * nc
    width = ntp * BLOCK
    ctx_line = ny * CTX_DEV
    z, y, x, c = (lax.axis_index(a) for a in AXES)
    s = z * ny + y
    t = x * nc + c
    sib = 1 - c

    def line(axis, me, d, n):
        return {axis: lax.rem(me + d, n)}

    def tp_peer(dx, dc):
        return {"x": lax.rem(x + dx, nx), "c": lax.rem(c + dc, nc)}

    def sp_peer(step):
        p = lax.rem(s + step + nsp, nsp)
        return {"z": p // ny, "y": lax.rem(p, ny)}

    tp_steps = [(dx, dc) for dx in range(nx) for dc in range(nc) if (dx, dc) != (0, 0)]

    barrier = pltpu.get_barrier_semaphore()
    peers = [line("y", y, d, ny) for d in range(1, ny)]
    peers += [line("z", z, d, nz) for d in range(1, nz)]
    peers += [tp_peer(dx, dc) for dx, dc in tp_steps]
    peers += [sp_peer(1), sp_peer(-1)]
    for peer in peers:
        pl.semaphore_signal(barrier, inc=1, device_id=peer, device_id_type=MESH)

    def load(k, src, dst):
        cp = pltpu.make_async_copy(src, dst, load_sem.at[k])
        cp.start()
        return cp

    first_loads = [
        load(10, cond_hbm, cond),
        load(11, cond_ctx_hbm, cond_ctx),
        load(0, shift_w, wmod.at[0]),
        load(1, scale_w, wmod.at[1]),
        load(2, gate_w, wmod.at[2]),
    ]
    gain_load = load(12, norm_gain_hbm, norm_gain)
    ctx_load = load(3, context, craw.at[0])
    lat_load = load(4, latent, lat)
    bias_load = load(15, offset_bias_hbm, offset_bias)
    w_loads = [
        load(13, query_gain_hbm, query_gain),
        load(14, key_gain_hbm, key_gain),
        load(5, key_w, w_all.at[:, 0:LANE]),
        load(6, value_w, w_all.at[:, LANE : 2 * LANE]),
        load(7, query_w, w_all.at[:, 2 * LANE : 3 * LANE]),
    ]
    late_loads = [
        load(8, latent.at[:, pl.ds(pl.multiple_of(t * BLOCK, BLOCK), BLOCK)], own),
        load(9, out_w, wo),
    ]

    for cp in first_loads:
        cp.wait()
    act = silu(cond[...].astype(F32)).astype(BF16)
    act_ctx = silu(cond_ctx[...].astype(F32)).astype(BF16)
    acts = jnp.concatenate([act, act_ctx], axis=0)
    p_shift = dot(acts, wmod[0])
    p_scale = dot(acts, wmod[1])
    p_gate = dot(acts, wmod[2])
    half = BLOCK // 2
    m1[0, 0:2, :] = p_shift[:, :half]
    m1[0, 2:4, :] = p_scale[:, :half]
    m1[0, 4:6, :] = p_shift[:, half:]
    m1[0, 6:8, :] = p_scale[:, half:]
    g1[0, 0:2, :] = p_gate[:, :half]
    g1[0, 2:4, :] = p_gate[:, half:]
    g1[0, 4:8, :] = jnp.zeros((4, half), F32)
    ctx_load.wait()
    pl.semaphore_wait(barrier, len(peers))

    def remote(src, dst, send, recv, peer):
        return pltpu.make_async_remote_copy(
            src_ref=src,
            dst_ref=dst,
            send_sem=send,
            recv_sem=recv,
            device_id=peer,
            device_id_type=MESH,
        )

    sent = []

    def send_line(axis, me, n, src, dst_of, send, recv):
        copies = {}
        for d in far_first(n):
            cp = remote(src, dst_of(d), send.at[d], recv.at[d], line(axis, me, d, n))
            cp.start()
            copies[d] = cp
        sent.extend(copies.values())
        return copies

    p1 = send_line("y", y, ny, m1.at[0], lambda d: m1.at[d], s1, r1)
    pc = send_line("y", y, ny, craw.at[0], lambda d: craw.at[d], sc, rc)
    pg1 = send_line("y", y, ny, g1.at[0], lambda d: g1.at[d], sg1, rg1)

    gain_load.wait()
    for b in range(width // LANE):
        gain_row[0:1, b * LANE : (b + 1) * LANE] = norm_gain[b : b + 1, :].astype(F32)
    gain = gain_row[...]
    lat_load.wait()

    def norm_rows(i, carry):
        rows = pl.ds(pl.multiple_of(i * 16, 16), 16)
        v = lat[rows, :].astype(F32)
        r = lax.rsqrt(jnp.mean(v * v, axis=-1, keepdims=True) + EPS)
        xn[rows, :] = v * r * gain
        return carry

    lax.fori_loop(0, TOK // 16, norm_rows, 0)

    for cp in p1.values():
        cp.wait_recv()
    total = m1[0]
    for d in range(1, ny):
        total = total + m1[d]
    m2[0] = total
    p2 = send_line("z", z, nz, m2.at[0], lambda d: m2.at[d], s2, r2)

    bias_load.wait()
    bias_rows[...] = jnp.zeros(bias_rows.shape, F32)
    for h in range(2):
        bias_rows[h, 0 : 2 * WIN_ROWS - 1, 0 : 2 * WIN_COLS - 1] = offset_bias[:, h, :]
    kv[:, 2 * LANE :] = jnp.ones((3 * TOK, LANE), BF16)
    kvc[:, 2 * LANE :] = jnp.ones((kvc.shape[0], LANE), BF16)
    q_col = lax.broadcasted_iota(jnp.int32, (GRID_W, LANE), 0)
    lane = lax.broadcasted_iota(jnp.int32, (GRID_W, LANE), 1)
    k_col = lax.rem(lane, GRID_W)
    k_row = lane // GRID_W
    first_col = jnp.clip(q_col - WIN_COLS // 2, 0, GRID_W - WIN_COLS)
    col_ok = (k_col >= first_col) & (k_col < first_col + WIN_COLS)
    for h in range(2):
        table_rows = bias_rows[h]
        pairs = table_rows[0:15] + pltpu.roll(table_rows, GRID_W, 1)[1:16]
        toeplitz = {}
        for ro in range(14):
            spread = jnp.broadcast_to(pairs[ro : ro + 1], (GRID_W, LANE))
            toeplitz[ro] = pltpu.roll(
                spread, LANE - (WIN_COLS - 1), 1, stride=1, stride_axis=0
            )
        for r in range(ROWS):
            begin = jnp.where(s == 0, ROWS, jnp.where(s == nsp - 1, 0, r))
            rows = pl.ds(h * TOK + r * GRID_W, GRID_W)
            high = None
            tiles = []
            for kp in range(6):
                row = k_row + 2 * kp
                ok = col_ok & (row >= begin) & (row < begin + WIN_ROWS)
                tile = jnp.where(ok, toeplitz[2 * kp - r + 3], NEG)
                tiles.append(tile)
                high = tile if high is None else jnp.maximum(high, tile)
            peak = jnp.max(high, axis=-1, keepdims=True)
            top[rows, :] = jnp.broadcast_to(peak * LOG2E, (GRID_W, LANE))
            for kp in range(6):
                table[rows, kp * LANE : (kp + 1) * LANE] = (tiles[kp] - peak) * LOG2E

    for cp in p2.values():
        cp.wait_recv()
    total = m2[0]
    for d in range(1, nz):
        total = total + m2[d]
    mod[t] = total
    p3 = {}
    for dx, dc in tp_steps:
        k = dx * nc + dc
        cp = remote(mod.at[t], mod.at[t], s3.at[k], r3.at[k], tp_peer(dx, dc))
        cp.start()
        sent.append(cp)
        src = lax.rem(x + nx - dx, nx) * nc + lax.rem(c + nc - dc, nc)
        p3[k] = remote(mod.at[src], mod.at[src], s3.at[k], r3.at[k], tp_peer(dx, dc))

    for cp in pc.values():
        cp.wait_recv()
    for d in range(ny):
        v = craw[d].astype(F32)
        r = lax.rsqrt(jnp.mean(v * v, axis=-1, keepdims=True) + EPS)
        cxn[d * CTX_DEV : (d + 1) * CTX_DEV, :] = v * r * gain
    for cp in pg1.values():
        cp.wait_recv()
    total = g1[0]
    for d in range(1, ny):
        total = total + g1[d]
    g2[0] = total
    pg2 = send_line("z", z, nz, g2.at[0], lambda d: g2.at[d], sg2, rg2)

    row_head = lax.broadcasted_iota(jnp.int32, (LANE, LANE), 0) // HEAD_DIM
    col_head = lax.broadcasted_iota(jnp.int32, (LANE, LANE), 1) // HEAD_DIM
    ones_block = jnp.where(row_head == col_head, 1.0 / HEAD_DIM, 0.0).astype(BF16)
    for cp in w_loads:
        cp.wait()
    kg = key_gain[...].astype(F32)
    qg = query_gain[...].astype(F32) * (HEAD_DIM**-0.5 * LOG2E)
    gains[0:1, 0:HEAD_DIM] = kg
    gains[0:1, HEAD_DIM:LANE] = kg
    gains[1:2, 0:HEAD_DIM] = qg
    gains[1:2, HEAD_DIM:LANE] = qg

    for cp in p3.values():
        cp.wait_recv()

    def vec(block, which):
        return jnp.concatenate([mod[block, which : which + 1, :], mod[block, which + 4 : which + 5, :]], axis=1)

    for b in range(ntp):
        cols = slice(b * BLOCK, (b + 1) * BLOCK)
        chid[:, cols] = (cxn[:, cols] * (1.0 + vec(b, 3)) + vec(b, 1)).astype(BF16)
    raw = dot(chid[...], w_all[:, 0 : 2 * LANE])
    kvc[0:ctx_line, 0:LANE] = (head_norm(raw[:, :LANE], ones_block) * gains[0:1, :]).astype(BF16)
    kvc[0:ctx_line, LANE : 2 * LANE] = raw[:, LANE:].astype(BF16)
    order = near_first(nz)
    place = {d: order.index(d) * ctx_line for d in order}

    def kvc_at(d):
        return kvc.at[place[d] : place[d] + ctx_line, 0 : 2 * LANE]

    pk = send_line("z", z, nz, kvc_at(0), kvc_at, sk, rk)

    for b in range(ntp):
        cols = slice(b * BLOCK, (b + 1) * BLOCK)
        hid[:, cols] = (xn[:, cols] * (1.0 + vec(b, 2)) + vec(b, 0)).astype(BF16)
    raw = dot(hid[...], w_all[:, 0 : 2 * LANE])
    kv[TOK : 2 * TOK, 0:LANE] = (head_norm(raw[:, :LANE], ones_block) * gains[0:1, :]).astype(BF16)
    kv[TOK : 2 * TOK, LANE : 2 * LANE] = raw[:, LANE:].astype(BF16)
    mine = kv.at[TOK : 2 * TOK, 0 : 2 * LANE]
    up = remote(mine, kv.at[0:TOK, 0 : 2 * LANE], sh.at[0], rh.at[0], sp_peer(1))
    down = remote(mine, kv.at[2 * TOK : 3 * TOK, 0 : 2 * LANE], sh.at[1], rh.at[1], sp_peer(-1))
    up.start()
    down.start()
    sent.extend([up, down])

    raw = dot(hid[...], w_all[:, 2 * LANE : 3 * LANE])
    queries = head_norm(raw, ones_block) * gains[1:2, :]
    head_of = lax.broadcasted_iota(jnp.int32, (TOK, LANE), 1) // HEAD_DIM
    for h in range(2):
        qm[h] = jnp.where(head_of == h, queries, 0.0).astype(BF16)

    def window(block, start):
        rows = slice(block * TOK, (block + 1) * TOK)
        for h in range(2):
            sc_ = dot_nt(qm[h], kv[rows, 0:LANE])
            w = jnp.exp2(sc_ + table[h * TOK : (h + 1) * TOK, rows]).astype(BF16)
            part = dot(w, kv[rows, LANE:])
            acc[h] = part if start else acc[h] + part

    def prefix(lo, hi):
        for h in range(2):
            sc_ = dot_nt(qm[h], kvc[lo:hi, 0:LANE])
            peak = top[h * TOK : (h + 1) * TOK, :]
            if hi - lo >= LANE:
                peak = jnp.concatenate([peak] * ((hi - lo) // LANE), axis=1)
            else:
                peak = peak[:, : hi - lo]
            w = jnp.exp2(sc_ - peak).astype(BF16)
            acc[h] = acc[h] + dot(w, kvc[lo:hi, LANE:])

    window(1, True)
    up.wait_recv()
    window(0, False)
    down.wait_recv()
    window(2, False)
    per = max(1, min(BLOCK // ctx_line, nz))
    for g in range(0, nz, per):
        for d in order[g : g + per]:
            if d:
                pk[d].wait_recv()
        prefix(g * ctx_line, (g + per) * ctx_line)

    parts = []
    for h in range(2):
        full = acc[h]
        parts.append(full[:, :LANE] / full[:, LANE:])
    mx[0, c] = jnp.where(head_of == 0, parts[0], parts[1]).astype(BF16)

    mine = mx.at[0, c]
    pm = {}
    for dx in far_first(nx):
        cp = remote(mine, mx.at[dx, c], sm.at[dx], rm.at[dx], tp_peer(dx, 0))
        cp.start()
        pm[dx] = cp
    sent.extend(pm.values())
    pf = {}
    for dx in range(nx):
        pf[dx] = remote(mx.at[dx, c], mx.at[dx, c], sf.at[dx], rf.at[dx], {"c": sib})
    got = {dx: remote(mx.at[dx, sib], mx.at[dx, sib], sf.at[dx], rf.at[dx], {"c": sib}) for dx in range(nx)}
    pf[0].start()
    sent.extend(pf.values())

    for cp in pg2.values():
        cp.wait_recv()
    total = g2[0]
    for d in range(1, nz):
        total = total + g2[d]
    gate = jnp.concatenate([total[0:1], total[2:3]], axis=1)
    for cp in late_loads:
        cp.wait()
    for dx in sorted(range(1, nx), key=lambda d: min(d, nx - d)):
        pm[dx].wait_recv()
        pf[dx].start()
    proj = None
    for dx in [0] + sorted(range(1, nx), key=lambda d: min(d, nx - d)):
        got[dx].wait_recv()
        src = lax.rem(x + nx - dx, nx)
        rows = pl.ds(pl.multiple_of(src * 2 * LANE, 2 * LANE), 2 * LANE)
        part = dot(jnp.concatenate([mx[dx, 0], mx[dx, 1]], axis=1), wo[rows, :])
        proj = part if proj is None else proj + part
    out[...] = (own[...].astype(F32) + gate * proj).astype(BF16)
    for cp in sent:
        cp.wait_send()


def solution(mesh):
    nsp, ntp = mesh.devices.shape
    sizes = SIZES if SIZES else (8, nsp // 8, ntp // 2, 2)
    nz, ny, nx, nc = sizes
    split = Mesh(mesh.devices.reshape(sizes), AXES)
    sp, tp = ("z", "y"), ("x", "c")
    placed = (
        P(sp, None),
        P(sp, None),
        P(sp),
        P(sp),
        P(sp, tp),
        P(sp, tp),
        P(sp, tp),
        P(),
        P(None, tp),
        P(None, tp),
        P(None, tp),
        P(),
        P(),
        P(tp, None, None),
        P(None, tp),
    )
    width = ntp * BLOCK
    ctx_line = ny * CTX_DEV
    dma = pltpu.SemaphoreType.DMA
    vm = pltpu.VMEM

    def body(
        latent,
        context,
        cond,
        cond_ctx,
        shift_w,
        scale_w,
        gate_w,
        norm_gain,
        query_w,
        key_w,
        value_w,
        query_gain,
        key_gain,
        offset_bias,
        out_w,
    ):
        args = [
            latent,
            context,
            cond.reshape(1, -1),
            cond_ctx.reshape(1, -1),
            shift_w,
            scale_w,
            gate_w,
            norm_gain.reshape(-1, LANE),
            query_w,
            key_w,
            value_w,
            query_gain.reshape(1, -1),
            key_gain.reshape(1, -1),
            jnp.transpose(offset_bias, (1, 0, 2)),
            out_w,
        ]
        specs = [pl.BlockSpec(memory_space=pltpu.HBM)] * len(args)
        small = [vm(args[i].shape, args[i].dtype) for i in SMALL]
        depth = shift_w.shape[0]
        scratch = [
            vm((TOK, width), BF16),
            vm((TOK, width), F32),
            vm((TOK, width), BF16),
            vm((width, 3 * LANE), BF16),
            vm((ntp * LANE, BLOCK), BF16),
            vm((TOK, BLOCK), BF16),
            vm((ny, CTX_DEV, width), BF16),
            vm((ctx_line, width), F32),
            vm((ctx_line, width), BF16),
            vm((3 * TOK, 3 * LANE), BF16),
            vm((nz * ctx_line, 3 * LANE), BF16),
            vm((2, TOK, LANE), BF16),
            vm((2 * TOK, 3 * TOK), F32),
            vm((2 * TOK, LANE), F32),
            vm((2, TOK, 2 * LANE), F32),
            vm((2, 16, LANE), F32),
            vm((2, LANE), F32),
            vm((1, width), F32),
            vm((3, depth, BLOCK), BF16),
            vm((ny, 8, LANE), F32),
            vm((nz, 8, LANE), F32),
            vm((ny, 8, LANE), F32),
            vm((nz, 8, LANE), F32),
            vm((ntp, 8, LANE), F32),
            vm((nx, 2, TOK, LANE), BF16),
            *small,
            dma((16,)),
            dma((ny,)),
            dma((ny,)),
            dma((nz,)),
            dma((nz,)),
            dma((ny,)),
            dma((ny,)),
            dma((nz,)),
            dma((nz,)),
            dma((ntp,)),
            dma((ntp,)),
            dma((ny,)),
            dma((ny,)),
            dma((nz,)),
            dma((nz,)),
            dma((2,)),
            dma((2,)),
            dma((nx,)),
            dma((nx,)),
            dma((nx,)),
            dma((nx,)),
        ]
        return pl.pallas_call(
            functools.partial(kernel, sizes),
            out_shape=jax.ShapeDtypeStruct((TOK, BLOCK), BF16),
            in_specs=specs,
            out_specs=pl.BlockSpec(memory_space=pltpu.VMEM),
            scratch_shapes=scratch,
            compiler_params=pltpu.CompilerParams(
                collective_id=0, has_side_effects=True, vmem_limit_bytes=63 * 1024 * 1024
            ),
            name="fused_layer",
        )(*args)

    return jax.shard_map(body, mesh=split, in_specs=placed, out_specs=P(sp, tp), check_vma=False)


SIZES = None
```

```python
import functools
import math

import jax
import jax.numpy as jnp
from jax import lax
from jax.experimental import pallas as pl
from jax.experimental.pallas import tpu as pltpu
from jax.sharding import Mesh
from jax.sharding import PartitionSpec as P

HEAD_DIM = 64
WIN_ROWS = 8
WIN_COLS = 16
GRID_W = 64
ROWS = 4
TOK = ROWS * GRID_W
LANE = 2 * HEAD_DIM
BLOCK = 256
CTX_DEV = 8
EPS = 1e-06
LOG2E = math.log2(math.e)
NEG = -1e30
SMALL = (2, 3, 7, 11, 12, 13)
AXES = ("z", "y", "x", "c")
MESH = pl.DeviceIdType.MESH
F32 = jnp.float32
BF16 = jnp.bfloat16


CLASS_FROM = ((0, 0), (1, 0), (-1, 0), (0, 1), (2, 0), (-2, 0), (1, -1), (-1, 1))
CLASS = 8


def far_first(n):
    return sorted(range(1, n), key=lambda d: -min(d, n - d))


def near_first(n):
    return [0] + sorted(range(1, n), key=lambda d: min(d, n - d))


def dot(a, b):
    return jnp.dot(a, b, preferred_element_type=F32)


def dot_nt(a, b):
    return lax.dot_general(a, b, (((1,), (1,)), ((), ())), preferred_element_type=F32)


def silu(v):
    return v / (1.0 + jnp.exp(-v))


def head_norm(raw, ones_block):
    sq = raw * raw
    hi = sq.astype(BF16)
    lo = (sq - hi.astype(F32)).astype(BF16)
    return raw * lax.rsqrt(dot(hi, ones_block) + dot(lo, ones_block) + EPS)


def kernel(
    sizes,
    latent,
    context,
    cond_hbm,
    cond_ctx_hbm,
    shift_w,
    scale_w,
    gate_w,
    norm_gain_hbm,
    query_w,
    key_w,
    value_w,
    query_gain_hbm,
    key_gain_hbm,
    offset_bias_hbm,
    out_w,
    out,
    lat,
    xn,
    hid,
    w_all,
    wo,
    own,
    craw,
    cxn,
    chid,
    kv,
    kvc,
    qm,
    table,
    top,
    acc,
    bias_rows,
    gains,
    gain_row,
    wmod,
    m1,
    m2,
    g1,
    g2,
    mod,
    mx,
    cond,
    cond_ctx,
    norm_gain,
    query_gain,
    key_gain,
    offset_bias,
    load_sem,
    s1,
    r1,
    s2,
    r2,
    sg1,
    rg1,
    sg2,
    rg2,
    s3,
    r3,
    sc,
    rc,
    sk,
    rk,
    sh,
    rh,
    sm,
    rm,
    sf,
    rf,
):
    scope = [None]

    def phase(name):
        if scope[0] is not None:
            scope[0].__exit__(None, None, None)
        scope[0] = jax.named_scope(name) if name else None
        if name:
            scope[0].__enter__()

    nz, ny, nx, nc = sizes
    nsp, ntp = nz * ny, nx * nc
    width = ntp * BLOCK
    ctx_line = CLASS * CTX_DEV
    z, y, x, c = (lax.axis_index(a) for a in AXES)
    s = z * ny + y
    t = x * nc + c
    sib = 1 - c

    def line(axis, me, d, n):
        return {axis: lax.rem(me + d, n)}

    def tp_peer(dx, dc):
        return {"x": lax.rem(x + dx, nx), "c": lax.rem(c + dc, nc)}

    def sp_peer(step):
        p = lax.rem(s + step + nsp, nsp)
        return {"z": p // ny, "y": lax.rem(p, ny)}

    tp_steps = [(dx, dc) for dx in range(nx) for dc in range(nc) if (dx, dc) != (0, 0)]

    phase("greet")
    barrier = pltpu.get_barrier_semaphore()
    peers = [line("y", y, d, ny) for d in range(1, ny)]
    peers += [line("z", z, d, nz) for d in range(1, nz)]
    peers += [tp_peer(dx, dc) for dx, dc in tp_steps]
    peers += [sp_peer(1), sp_peer(-1)]
    for peer in peers:
        pl.semaphore_signal(barrier, inc=1, device_id=peer, device_id_type=MESH)

    def load(k, src, dst):
        cp = pltpu.make_async_copy(src, dst, load_sem.at[k])
        cp.start()
        return cp

    first_loads = [
        load(10, cond_hbm, cond),
        load(11, cond_ctx_hbm, cond_ctx),
        load(0, shift_w, wmod.at[0]),
        load(1, scale_w, wmod.at[1]),
        load(2, gate_w, wmod.at[2]),
    ]
    gain_load = load(12, norm_gain_hbm, norm_gain)
    ctx_load = load(3, context, craw.at[0])
    lat_load = load(4, latent, lat)
    bias_load = load(15, offset_bias_hbm, offset_bias)
    w_loads = [
        load(13, query_gain_hbm, query_gain),
        load(14, key_gain_hbm, key_gain),
        load(5, key_w, w_all.at[:, 0:LANE]),
        load(6, value_w, w_all.at[:, LANE : 2 * LANE]),
        load(7, query_w, w_all.at[:, 2 * LANE : 3 * LANE]),
    ]
    late_loads = [
        load(8, latent.at[:, pl.ds(pl.multiple_of(t * BLOCK, BLOCK), BLOCK)], own),
        load(9, out_w, wo),
    ]

    phase("partial")
    for cp in first_loads:
        cp.wait()
    act = silu(cond[...].astype(F32)).astype(BF16)
    act_ctx = silu(cond_ctx[...].astype(F32)).astype(BF16)
    acts = jnp.concatenate([act, act_ctx], axis=0)
    p_shift = dot(acts, wmod[0])
    p_scale = dot(acts, wmod[1])
    p_gate = dot(acts, wmod[2])
    half = BLOCK // 2
    m1[0, 0:2, :] = p_shift[:, :half]
    m1[0, 2:4, :] = p_scale[:, :half]
    m1[0, 4:6, :] = p_shift[:, half:]
    m1[0, 6:8, :] = p_scale[:, half:]
    g1[0, 0:2, :] = p_gate[:, :half]
    g1[0, 2:4, :] = p_gate[:, half:]
    g1[0, 4:8, :] = jnp.zeros((4, half), F32)
    ctx_load.wait()
    phase("barrier")
    pl.semaphore_wait(barrier, len(peers))

    def remote(src, dst, send, recv, peer):
        return pltpu.make_async_remote_copy(
            src_ref=src,
            dst_ref=dst,
            send_sem=send,
            recv_sem=recv,
            device_id=peer,
            device_id_type=MESH,
        )

    sent = []

    def send_line(axis, me, n, src, dst_of, send, recv):
        copies = {}
        for d in far_first(n):
            cp = remote(src, dst_of(d), send.at[d], recv.at[d], line(axis, me, d, n))
            cp.start()
            copies[d] = cp
        sent.extend(copies.values())
        return copies

    phase("send1")
    p1 = send_line("y", y, ny, m1.at[0], lambda d: m1.at[d], s1, r1)
    half_cols = pl.ds(pl.multiple_of(c * (width // 2), width // 2), width // 2)

    def raw_at(slot):
        return craw.at[slot, :, half_cols]

    across = remote(raw_at(0), raw_at(CLASS), sc.at[0], rc.at[0], line("z", z, nz // 2, nz))
    across.start()
    sent.append(across)

    phase("norm")
    gain_load.wait()
    for b in range(width // LANE):
        gain_row[0:1, b * LANE : (b + 1) * LANE] = norm_gain[b : b + 1, :].astype(F32)
    gain = gain_row[...]
    lat_load.wait()

    def norm_rows(i, carry):
        rows = pl.ds(pl.multiple_of(i * 16, 16), 16)
        v = lat[rows, :].astype(F32)
        r = lax.rsqrt(jnp.mean(v * v, axis=-1, keepdims=True) + EPS)
        xn[rows, :] = v * r * gain
        return carry

    lax.fori_loop(0, TOK // 16, norm_rows, 0)

    phase("wait1")
    for cp in p1.values():
        cp.wait_recv()
    total = m1[0]
    for d in range(1, ny):
        total = total + m1[d]
    m2[0] = total
    p2 = send_line("z", z, nz, m2.at[0], lambda d: m2.at[d], s2, r2)

    phase("bias")
    across.wait_recv()
    pc = []
    for d in (4, 3, 5, 2, 6, 1, 7):
        slot = d // 2 if d % 2 == 0 else 4 + d // 2
        src = raw_at(0) if d % 2 == 0 else raw_at(CLASS)
        cp = remote(src, raw_at(slot), sc.at[d], rc.at[d], line("y", y, d, ny))
        cp.start()
        pc.append(cp)
    sent.extend(pc)
    pg1 = send_line("y", y, ny, g1.at[0], lambda d: g1.at[d], sg1, rg1)

    bias_load.wait()
    bias_rows[...] = jnp.zeros(bias_rows.shape, F32)
    for h in range(2):
        bias_rows[h, 0 : 2 * WIN_ROWS - 1, 0 : 2 * WIN_COLS - 1] = offset_bias[:, h, :]
    kv[:, 2 * LANE :] = jnp.ones((3 * TOK, LANE), BF16)
    kvc[:, 2 * LANE :] = jnp.ones((kvc.shape[0], LANE), BF16)

    def clear(when, lo, hi):
        @pl.when(when)
        def _():
            kv[lo:hi, 0 : 2 * LANE] = jnp.zeros((hi - lo, 2 * LANE), BF16)

    clear(s == 0, 0, TOK)
    clear(s == nsp - 1, 2 * TOK, 3 * TOK - GRID_W)
    clear(s != 0, 3 * TOK - GRID_W, 3 * TOK)
    q_col = lax.broadcasted_iota(jnp.int32, (GRID_W, LANE), 0)
    lane = lax.broadcasted_iota(jnp.int32, (GRID_W, LANE), 1)
    k_col = lax.rem(lane, GRID_W)
    k_row = lane // GRID_W
    first_col = jnp.clip(q_col - WIN_COLS // 2, 0, GRID_W - WIN_COLS)
    col_ok = (k_col >= first_col) & (k_col < first_col + WIN_COLS)
    for h in range(2):
        table_rows = bias_rows[h]
        pairs = table_rows[0:15] + pltpu.roll(table_rows, GRID_W, 1)[1:16]
        toeplitz = {}
        for ro in range(14):
            spread = jnp.broadcast_to(pairs[ro : ro + 1], (GRID_W, LANE))
            toeplitz[ro] = pltpu.roll(
                spread, LANE - (WIN_COLS - 1), 1, stride=1, stride_axis=0
            )
        for r in range(ROWS):
            begin = jnp.where(s == 0, ROWS, jnp.where(s == nsp - 1, 0, r))
            rows = pl.ds(h * TOK + r * GRID_W, GRID_W)
            high = None
            tiles = []
            for kp in range(6):
                row = k_row + 2 * kp
                ok = col_ok & (row >= begin) & (row < begin + WIN_ROWS)
                tile = jnp.where(ok, toeplitz[2 * kp - r + 3], NEG)
                tiles.append(tile)
                high = tile if high is None else jnp.maximum(high, tile)
            peak = jnp.max(high, axis=-1, keepdims=True)
            top[rows, :] = jnp.broadcast_to(peak * LOG2E, (GRID_W, LANE))
            for kp in range(6):
                table[rows, kp * LANE : (kp + 1) * LANE] = (tiles[kp] - peak) * LOG2E

    phase("wait2")
    for cp in p2.values():
        cp.wait_recv()
    total = m2[0]
    for d in range(1, nz):
        total = total + m2[d]
    mod[t] = total
    p3 = {}
    for dx, dc in tp_steps:
        k = dx * nc + dc
        cp = remote(mod.at[t], mod.at[t], s3.at[k], r3.at[k], tp_peer(dx, dc))
        cp.start()
        sent.append(cp)
        src = lax.rem(x + nx - dx, nx) * nc + lax.rem(c + nc - dc, nc)
        p3[k] = remote(mod.at[src], mod.at[src], s3.at[k], r3.at[k], tp_peer(dx, dc))

    phase("ctxnorm")
    phase("gate1")
    for cp in pg1.values():
        cp.wait_recv()
    total = g1[0]
    for d in range(1, ny):
        total = total + g1[d]
    g2[0] = total
    pg2 = send_line("z", z, nz, g2.at[0], lambda d: g2.at[d], sg2, rg2)

    row_head = lax.broadcasted_iota(jnp.int32, (LANE, LANE), 0) // HEAD_DIM
    col_head = lax.broadcasted_iota(jnp.int32, (LANE, LANE), 1) // HEAD_DIM
    ones_block = jnp.where(row_head == col_head, 1.0 / HEAD_DIM, 0.0).astype(BF16)
    for cp in w_loads:
        cp.wait()
    kg = key_gain[...].astype(F32)
    qg = query_gain[...].astype(F32) * (HEAD_DIM**-0.5 * LOG2E)
    gains[0:1, 0:HEAD_DIM] = kg
    gains[0:1, HEAD_DIM:LANE] = kg
    gains[1:2, 0:HEAD_DIM] = qg
    gains[1:2, HEAD_DIM:LANE] = qg

    phase("wait3")
    for cp in p3.values():
        cp.wait_recv()

    phase("ctxfwd")
    for cp in pc:
        cp.wait_recv()
    sib_cols = pl.ds(pl.multiple_of(sib * (width // 2), width // 2), width // 2)
    halves = [craw.at[1:CLASS, :, cols] for cols in (half_cols, sib_cols)]
    cross = remote(halves[0], halves[0], sc.at[8], rc.at[8], {"c": sib})
    crossed = remote(halves[1], halves[1], sc.at[8], rc.at[8], {"c": sib})
    cross.start()
    sent.append(cross)

    def vec(block, which):
        return jnp.concatenate([mod[block, which : which + 1, :], mod[block, which + 4 : which + 5, :]], axis=1)

    phase("kv")
    for b in range(ntp):
        cols = slice(b * BLOCK, (b + 1) * BLOCK)
        hid[:, cols] = (xn[:, cols] * (1.0 + vec(b, 2)) + vec(b, 0)).astype(BF16)
    raw = dot(hid[...], w_all[:, 0 : 2 * LANE])
    kv[TOK : 2 * TOK, 0:LANE] = (head_norm(raw[:, :LANE], ones_block) * gains[0:1, :]).astype(BF16)
    kv[TOK : 2 * TOK, LANE : 2 * LANE] = raw[:, LANE:].astype(BF16)
    def kv_rows(lo, hi):
        return kv.at[lo:hi, 0 : 2 * LANE]

    short = TOK - GRID_W
    up = remote(kv_rows(TOK, 2 * TOK), kv_rows(0, TOK), sh.at[0], rh.at[0], sp_peer(1))
    down = remote(kv_rows(TOK, TOK + short), kv_rows(2 * TOK, 2 * TOK + short), sh.at[1], rh.at[1], sp_peer(-1))
    last = remote(kv_rows(TOK + short, 2 * TOK), kv_rows(2 * TOK + short, 3 * TOK), sh.at[2], rh.at[2], sp_peer(-1))
    pl.when(s < nsp - 1)(up.start)
    pl.when(s > 0)(down.start)
    pl.when(s == 1)(last.start)

    phase("ctxkv")
    crossed.wait_recv()
    for d in range(CLASS):
        v = craw[d].astype(F32)
        r = lax.rsqrt(jnp.mean(v * v, axis=-1, keepdims=True) + EPS)
        cxn[d * CTX_DEV : (d + 1) * CTX_DEV, :] = v * r * gain
    for b in range(ntp):
        cols = slice(b * BLOCK, (b + 1) * BLOCK)
        chid[:, cols] = (cxn[:, cols] * (1.0 + vec(b, 3)) + vec(b, 1)).astype(BF16)
    raw = dot(chid[...], w_all[:, 0 : 2 * LANE])
    kvc[0:ctx_line, 0:LANE] = (head_norm(raw[:, :LANE], ones_block) * gains[0:1, :]).astype(BF16)
    kvc[0:ctx_line, LANE : 2 * LANE] = raw[:, LANE:].astype(BF16)

    def kvc_at(k):
        return kvc.at[k * ctx_line : (k + 1) * ctx_line, 0 : 2 * LANE]

    pk = {}
    for k in (4, 5, 6, 7, 1, 2, 3):
        oz, oy = CLASS_FROM[k]
        peer = {"z": lax.rem(z - oz + nz, nz), "y": lax.rem(y - oy + ny, ny)}
        pk[k] = remote(kvc_at(0), kvc_at(k), sk.at[k], rk.at[k], peer)
        pk[k].start()
    sent.extend(pk.values())

    phase("q")
    raw = dot(hid[...], w_all[:, 2 * LANE : 3 * LANE])
    queries = head_norm(raw, ones_block) * gains[1:2, :]
    head_of = lax.broadcasted_iota(jnp.int32, (TOK, LANE), 1) // HEAD_DIM
    for h in range(2):
        qm[h] = jnp.where(head_of == h, queries, 0.0).astype(BF16)

    def window(block, start):
        rows = slice(block * TOK, (block + 1) * TOK)
        for h in range(2):
            sc_ = dot_nt(qm[h], kv[rows, 0:LANE])
            w = jnp.exp2(sc_ + table[h * TOK : (h + 1) * TOK, rows]).astype(BF16)
            part = dot(w, kv[rows, LANE:])
            acc[h] = part if start else acc[h] + part

    def prefix(lo, hi):
        for h in range(2):
            sc_ = dot_nt(qm[h], kvc[lo:hi, 0:LANE])
            peak = top[h * TOK : (h + 1) * TOK, :]
            if hi - lo >= LANE:
                peak = jnp.concatenate([peak] * ((hi - lo) // LANE), axis=1)
            else:
                peak = peak[:, : hi - lo]
            w = jnp.exp2(sc_ - peak).astype(BF16)
            acc[h] = acc[h] + dot(w, kvc[lo:hi, LANE:])

    phase("attn_own")
    window(1, True)
    phase("attn_up")
    pl.when(s > 0)(up.wait_recv)
    window(0, False)
    phase("attn_down")
    pl.when(s < nsp - 1)(down.wait_recv)
    pl.when(s == 0)(last.wait_recv)
    window(2, False)
    phase("attn_near")
    for k in (1, 2, 3):
        pk[k].wait_recv()
    prefix(0, 4 * ctx_line)
    phase("attn_far")
    for k in (4, 5, 6, 7):
        pk[k].wait_recv()
    prefix(4 * ctx_line, CLASS * ctx_line)

    phase("mixed")
    parts = []
    for h in range(2):
        full = acc[h]
        parts.append(full[:, :LANE] / full[:, LANE:])
    mx[0, c] = jnp.where(head_of == 0, parts[0], parts[1]).astype(BF16)

    mine = mx.at[0, c]
    pm = {}
    for dx in far_first(nx):
        cp = remote(mine, mx.at[dx, c], sm.at[dx], rm.at[dx], tp_peer(dx, 0))
        cp.start()
        pm[dx] = cp
    sent.extend(pm.values())
    pf = {}
    for dx in range(nx):
        pf[dx] = remote(mx.at[dx, c], mx.at[dx, c], sf.at[dx], rf.at[dx], {"c": sib})
    got = {dx: remote(mx.at[dx, sib], mx.at[dx, sib], sf.at[dx], rf.at[dx], {"c": sib}) for dx in range(nx)}
    pf[0].start()
    sent.extend(pf.values())

    phase("gate2")
    for cp in pg2.values():
        cp.wait_recv()
    total = g2[0]
    for d in range(1, nz):
        total = total + g2[d]
    gate = jnp.concatenate([total[0:1], total[2:3]], axis=1)
    for cp in late_loads:
        cp.wait()
    phase("forward")
    for dx in sorted(range(1, nx), key=lambda d: min(d, nx - d)):
        pm[dx].wait_recv()
        pf[dx].start()
    phase("proj")
    proj = None
    for dx in [0] + sorted(range(1, nx), key=lambda d: min(d, nx - d)):
        got[dx].wait_recv()
        src = lax.rem(x + nx - dx, nx)
        rows = pl.ds(pl.multiple_of(src * 2 * LANE, 2 * LANE), 2 * LANE)
        part = dot(jnp.concatenate([mx[dx, 0], mx[dx, 1]], axis=1), wo[rows, :])
        proj = part if proj is None else proj + part
    out[...] = (own[...].astype(F32) + gate * proj).astype(BF16)
    phase("drain")
    pl.when(s < nsp - 1)(up.wait_send)
    pl.when(s > 0)(down.wait_send)
    pl.when(s == 1)(last.wait_send)
    for cp in sent:
        cp.wait_send()
    phase(None)


def solution(mesh):
    nsp, ntp = mesh.devices.shape
    sizes = SIZES if SIZES else (8, nsp // 8, ntp // 2, 2)
    nz, ny, nx, nc = sizes
    split = Mesh(mesh.devices.reshape(sizes), AXES)
    sp, tp = ("z", "y"), ("x", "c")
    placed = (
        P(sp, None),
        P(sp, None),
        P(sp),
        P(sp),
        P(sp, tp),
        P(sp, tp),
        P(sp, tp),
        P(),
        P(None, tp),
        P(None, tp),
        P(None, tp),
        P(),
        P(),
        P(tp, None, None),
        P(None, tp),
    )
    width = ntp * BLOCK
    ctx_line = CLASS * CTX_DEV
    dma = pltpu.SemaphoreType.DMA
    vm = pltpu.VMEM

    def body(
        latent,
        context,
        cond,
        cond_ctx,
        shift_w,
        scale_w,
        gate_w,
        norm_gain,
        query_w,
        key_w,
        value_w,
        query_gain,
        key_gain,
        offset_bias,
        out_w,
    ):
        args = [
            latent,
            context,
            cond.reshape(1, -1),
            cond_ctx.reshape(1, -1),
            shift_w,
            scale_w,
            gate_w,
            norm_gain.reshape(-1, LANE),
            query_w,
            key_w,
            value_w,
            query_gain.reshape(1, -1),
            key_gain.reshape(1, -1),
            jnp.transpose(offset_bias, (1, 0, 2)),
            out_w,
        ]
        specs = [pl.BlockSpec(memory_space=pltpu.HBM)] * len(args)
        small = [vm(args[i].shape, args[i].dtype) for i in SMALL]
        depth = shift_w.shape[0]
        scratch = [
            vm((TOK, width), BF16),
            vm((TOK, width), F32),
            vm((TOK, width), BF16),
            vm((width, 3 * LANE), BF16),
            vm((ntp * LANE, BLOCK), BF16),
            vm((TOK, BLOCK), BF16),
            vm((CLASS + 1, CTX_DEV, width), BF16),
            vm((ctx_line, width), F32),
            vm((ctx_line, width), BF16),
            vm((3 * TOK, 3 * LANE), BF16),
            vm((CLASS * ctx_line, 3 * LANE), BF16),
            vm((2, TOK, LANE), BF16),
            vm((2 * TOK, 3 * TOK), F32),
            vm((2 * TOK, LANE), F32),
            vm((2, TOK, 2 * LANE), F32),
            vm((2, 16, LANE), F32),
            vm((2, LANE), F32),
            vm((1, width), F32),
            vm((3, depth, BLOCK), BF16),
            vm((ny, 8, LANE), F32),
            vm((nz, 8, LANE), F32),
            vm((ny, 8, LANE), F32),
            vm((nz, 8, LANE), F32),
            vm((ntp, 8, LANE), F32),
            vm((nx, 2, TOK, LANE), BF16),
            *small,
            dma((16,)),
            dma((ny,)),
            dma((ny,)),
            dma((nz,)),
            dma((nz,)),
            dma((ny,)),
            dma((ny,)),
            dma((nz,)),
            dma((nz,)),
            dma((ntp,)),
            dma((ntp,)),
            dma((CLASS + 1,)),
            dma((CLASS + 1,)),
            dma((CLASS,)),
            dma((CLASS,)),
            dma((3,)),
            dma((3,)),
            dma((nx,)),
            dma((nx,)),
            dma((nx,)),
            dma((nx,)),
        ]
        return pl.pallas_call(
            functools.partial(kernel, sizes),
            out_shape=pltpu.VMEM((TOK, BLOCK), BF16),
            in_specs=specs,
            out_specs=pl.BlockSpec(memory_space=pltpu.VMEM),
            scratch_shapes=scratch,
            compiler_params=pltpu.CompilerParams(
                collective_id=0, has_side_effects=True, vmem_limit_bytes=63 * 1024 * 1024
            ),
            name="fused_layer",
        )(*args)

    return jax.shard_map(body, mesh=split, in_specs=placed, out_specs=P(sp, tp), check_vma=False)


SIZES = None
```
